32 devices in a mesh: sp: 8 (over z, y), tp: 4 (over x, core).
Axes of the slice: x: 2, y: 2, z: 4, core: 2. Of those that a mesh axis runs over, the one named last changes fastest.
Arguments:
- queries: bfloat16 [8192, 8, 128], P('sp', 'tp'), may hold values from -160 to 160
- keys_values: bfloat16 [8192, 8, 128], P('sp', 'tp'), may hold values from -5 to 5
- sink_logits: float32 [8, 2], P('tp'), may hold values from 2 to 7
- doc_ids: int32 [8192], replicated, may hold values from 0 to 5, never falling along the last dimension, each value on 1 to 4096 neighbouring positions
- residual: bfloat16 [8192, 2048], P('sp'), may hold values from -6 to 6
- out_weight: bfloat16 [1024, 2048], P('tp'), may hold values from -1.5 to 1.5
- ffn_gain: float32 [2048], replicated, may hold values from 0.1 to 1.9
- gate_weight: bfloat16 [2048, 5120], P('sp', 'tp'), may hold values from -0.125 to 0.125
- value_weight: bfloat16 [2048, 5120], P('sp', 'tp'), may hold values from -0.125 to 0.125
- conv_taps: float32 [3, 5120], P(None, 'tp'), may hold values from -4 to 4
- down_weight: bfloat16 [2048, 5120], P('sp', 'tp'), may hold values from -0.078125 to 0.078125
Outputs:
- layer_out: bfloat16 [8192, 2048], P(('sp', 'tp'))
The draws below stay inside these ranges and needn't reach their ends.
Inputs may be any that keep to these rules, and one draw needn't show every extreme that they name: `doc_ids`: document numbers never fall along the sequence; a document spans at most 4096 positions.
All inputs are finite; a program needn't handle non-finite values.
Results may differ from the reference program's by a relative error of at most 0.02.
Values may be sent and summed in bfloat16 or wider, within the bound.
A program may use at most 128 MiB of HBM per device.

```python
import math
import jax
import jax.numpy as jnp
import numpy as np
from jax import lax

D = 2048
KV_HEADS = 8
GROUP = 2
HEAD_DIM = 64
ATTN = 1024
FF = 5120
WINDOW = 128
TOKENS = 8192
DOCS = 6
DOC_MOST = 4096
N_TP = 4


def drawn_pair(key):
    base = jax.random.fold_in(key, 4099)
    key_query, key_pairs = jax.random.split(base)
    pairs = jnp.clip(jax.random.normal(key_pairs, (TOKENS, KV_HEADS, 2 * HEAD_DIM), jnp.float32), -5.0, 5.0)
    asked = jnp.clip(jax.random.normal(key_query, (TOKENS, KV_HEADS, GROUP * HEAD_DIM), jnp.float32), -5.0, 5.0)
    return (asked, pairs)


def draw_queries(key, part):
    return drawn_pair(key)[0].astype(jnp.bfloat16)


def draw_keys_values(key, part):
    return drawn_pair(key)[1].astype(jnp.bfloat16)


def shard_levels(rng, dims, cuts, smallest, top_value):
    def one(axis_at, parts):
        draws = jax.random.uniform(jax.random.fold_in(jax.random.fold_in(rng, 6), axis_at), (parts,), jnp.float32, smallest / len(cuts), top_value / len(cuts))
        return jnp.repeat(jnp.exp(draws), dims[axis_at] // parts).reshape((-1,) + (1,) * (len(dims) - axis_at - 1))

    gain = one(*cuts[0])
    for cut in cuts[1:]:
        gain = gain * one(*cut)
    return gain


def split_up(count, total, bound, skew):
    loads = [(1 << 20) // math.isqrt(standing ** skew) + 1 for standing in range(2, count + 1)]
    surplus, counts = total - bound - (count - 1), [1] * (count - 1)
    while surplus > 0:
        candidates = [i for i in range(count - 1) if counts[i] < bound]
        mass, remaining = sum([loads[i] for i in candidates]), surplus
        for i in candidates:
            extra = min(bound - counts[i], max(1, remaining * loads[i] // mass), surplus)
            counts[i] = counts[i] + extra
            surplus = surplus - extra
    return np.array([bound] + counts)


def ragged(key, amount, total, bound, slope):
    if amount == 2:
        one = jax.random.randint(key, (), max(1, total - bound), min(bound, total - 1) + 1)
        return jnp.stack([one, total - one])
    tallies = jnp.asarray(split_up(amount, total, bound, slope), jnp.int32)
    pairs = (amount - 1) // 2
    source_of, sink = tallies[1:1 + 2 * pairs:2], tallies[2:2 + 2 * pairs:2]
    slack = jnp.minimum(source_of - 1, bound - sink)
    passed = jax.random.randint(jax.random.fold_in(key, 1), (pairs,), 0, 1 << 20) % (slack + 1)
    tallies = tallies.at[1:1 + 2 * pairs:2].set(source_of - passed).at[2:2 + 2 * pairs:2].set(sink + passed)
    return tallies[jax.random.permutation(jax.random.fold_in(key, 2), amount)]


def bell_draw(rng, extent, spread, limit, shards=(), held_as=jnp.bfloat16):
    factor_of = shard_levels(rng, extent, shards, -0.22, 0.18) if shards else 1.0
    values = jax.random.normal(rng, extent, jnp.float32) * spread * factor_of
    return jnp.minimum(jnp.maximum(values, -limit), limit).astype(held_as)


def setup_inputs(seed: int = 0) -> dict:
    streams_of = jax.random.split(jax.random.key(seed), 12)
    queries = draw_queries(jax.random.fold_in(streams_of[11], 71), 0)
    keys_values = draw_keys_values(jax.random.fold_in(streams_of[11], 71), 0)
    sink_logits = jnp.clip(2.0 + 5.0 * jax.random.uniform(streams_of[2], (KV_HEADS, GROUP), jnp.float32) ** shard_levels(streams_of[2], (KV_HEADS, GROUP), ((0, 4),), -0.2, 0.2), 2.0, 7.0)
    doc_ids = jnp.searchsorted(jnp.cumsum(ragged(streams_of[3], DOCS, TOKENS, DOC_MOST, 0)), jnp.arange(TOKENS), side="right").astype(jnp.int32)
    residual = bell_draw(streams_of[4], (TOKENS, D), 1.0, 6.0, ((0, 8),))
    out_weight = bell_draw(streams_of[5], (ATTN, D), (ATTN // 64) ** -0.5, 1.5, ((0, 4),))
    ffn_gain = jnp.clip(1.0 + 0.18 * jax.random.normal(streams_of[6], (D,), jnp.float32), 0.1, 1.9)
    gate_weight = bell_draw(streams_of[7], (D, FF), D ** -0.5, 0.125, ((0, 8), (1, 4)))
    value_weight = bell_draw(streams_of[8], (D, FF), D ** -0.5, 0.125, ((0, 8), (1, 4)))
    conv_taps = bell_draw(streams_of[9], (3, FF), 1.2, 4.0, ((1, 4),), jnp.float32)
    down_weight = bell_draw(streams_of[10], (D, FF), FF ** -0.5, 0.078125, ((0, 8), (1, 4)))
    return {"queries": queries, "keys_values": keys_values, "sink_logits": sink_logits, "doc_ids": doc_ids, "residual": residual, "out_weight": out_weight, "ffn_gain": ffn_gain, "gate_weight": gate_weight, "value_weight": value_weight, "conv_taps": conv_taps, "down_weight": down_weight}


norm_epsilon = 1e-06
masked_score = -1e+30
contract_last = (((1,), (1,)), ((), ()))

def rounded(values):
    return lax.optimization_barrier(values.astype(jnp.bfloat16)).astype(jnp.float32)

def band_blocks(padded, block_count, window_rows):
    row_block = padded.reshape((block_count + 2, window_rows) + padded.shape[1:])
    return jnp.concatenate([row_block[:-2], row_block[1:-1], row_block[2:]], axis=1)

def reference(queries, keys_values, sink_logits, doc_ids, residual, out_weight, ffn_gain, gate_weight, value_weight, conv_taps, down_weight):
    window_rows = WINDOW
    block_count = TOKENS // window_rows
    padded = jnp.pad(keys_values, ((window_rows, window_rows), (0, 0), (0, 0)))
    blocks = band_blocks(padded, block_count, window_rows)
    padded_docs = jnp.pad(doc_ids, window_rows, constant_values=-1)
    key_docs = band_blocks(padded_docs, block_count, window_rows)
    query_docs = doc_ids.reshape(block_count, window_rows)
    distance = jnp.arange(window_rows)[:, None] + window_rows - jnp.arange(3 * window_rows)[None, :]
    allowed = (jnp.abs(distance) <= WINDOW)[None] & (query_docs[:, :, None] == key_docs[:, None, :])
    query_blocks = queries.reshape(block_count, window_rows, KV_HEADS, GROUP, HEAD_DIM)

    def one_head(head):
        query_part = query_blocks[:, :, head].astype(jnp.float32)
        key_part = blocks[:, :, head, :HEAD_DIM].astype(jnp.float32)
        value_part = blocks[:, :, head, HEAD_DIM:].astype(jnp.float32)
        scores = jnp.einsum('nqgd,nsd->ngqs', query_part, key_part) * HEAD_DIM ** (-0.5)
        scores = jnp.where(allowed[:, None], scores, masked_score)
        sink_part = sink_logits[head].astype(jnp.float32)[None, :, None, None]
        top_score = jnp.maximum(lax.optimization_barrier(jnp.max(scores, axis=-1, keepdims=True)), sink_part)
        exp_scores = jnp.exp(scores - top_score)
        denominator = lax.optimization_barrier(jnp.sum(exp_scores, axis=-1, keepdims=True)) + jnp.exp(sink_part - top_score)
        probs = rounded(exp_scores / denominator)
        result = jnp.einsum('ngqs,nsd->nqgd', probs, value_part)
        return result.reshape(TOKENS, GROUP * HEAD_DIM)
    per_head = lax.map(one_head, jnp.arange(KV_HEADS))
    attended = jnp.transpose(per_head, (1, 0, 2)).reshape(TOKENS, ATTN).astype(jnp.bfloat16)
    share = ATTN // N_TP
    projected = jnp.zeros((TOKENS, D), jnp.float32)
    for shard in range(N_TP):
        partial_value = jnp.dot(attended[:, shard * share:(shard + 1) * share], out_weight[shard * share:(shard + 1) * share], preferred_element_type=jnp.float32)
        projected = projected + rounded(partial_value)
    stream = (residual.astype(jnp.float32) + projected).astype(jnp.bfloat16)
    stream_f = stream.astype(jnp.float32)
    scale = lax.rsqrt(lax.optimization_barrier(jnp.mean(stream_f * stream_f, axis=-1, keepdims=True)) + norm_epsilon)
    normed = (stream_f * scale * ffn_gain).astype(jnp.bfloat16)
    same_doc = (doc_ids[1:] == doc_ids[:-1]).astype(jnp.float32)
    prev_same = jnp.concatenate([jnp.zeros((1,), jnp.float32), same_doc])[:, None]
    next_same = jnp.concatenate([same_doc, jnp.zeros((1,), jnp.float32)])[:, None]
    hidden_share = FF // N_TP
    lowered = jnp.zeros((TOKENS, D), jnp.float32)
    for shard in range(N_TP):
        lo_col = shard * hidden_share
        hi_col = lo_col + hidden_share
        gate_pre = rounded(jnp.dot(normed, gate_weight[:, lo_col:hi_col], preferred_element_type=jnp.float32))
        value_pre = jnp.dot(normed, value_weight[:, lo_col:hi_col], preferred_element_type=jnp.float32)
        taps = conv_taps[:, lo_col:hi_col]
        before = jnp.pad(gate_pre, ((1, 0), (0, 0)))[:-1] * prev_same
        after = jnp.pad(gate_pre, ((0, 1), (0, 0)))[1:] * next_same
        conved = taps[0] * before + taps[1] * gate_pre + taps[2] * after
        hidden = (jax.nn.gelu(conved, approximate=True) * value_pre).astype(jnp.bfloat16)
        partial_value = lax.dot_general(hidden, down_weight[:, lo_col:hi_col], contract_last, preferred_element_type=jnp.float32)
        lowered = lowered + rounded(partial_value)
    return (stream_f + lowered).astype(jnp.bfloat16)
```

```python
import jax
import jax.numpy as jnp
from jax import lax
from jax.sharding import PartitionSpec as P

HEAD_DIM = 64
WINDOW = 128


norm_epsilon = 1e-06
masked_score = -1e30
contract_last = (((1,), (1,)), ((), ()))


def factors(count):
    inner = 1
    while count % (4 * inner * inner) == 0 or (inner == 1 and count % 2 == 0):
        inner *= 2
    return count // inner, inner


def ring_outer(cells, axis, outer, inner, by=1):
    pairs = [(o * inner + i, (o + by) % outer * inner + i) for o in range(outer) for i in range(inner)]
    return lax.ppermute(cells, axis, pairs)


def ring_inner(cells, axis, outer, inner, by=1):
    pairs = [(o * inner + i, o * inner + (i + by) % inner) for o in range(outer) for i in range(inner)]
    return lax.ppermute(cells, axis, pairs)


def later(cells, *arrived):
    return lax.optimization_barrier((cells,) + arrived)[0]


def gather_outer_first(block, axis, outer, inner, outer_after=(), inner_after=()):
    column = [block]
    for k in range(outer - 1):
        sent = later(block, *outer_after) if k == 0 and outer_after else column[-1]
        column.append(ring_outer(sent, axis, outer, inner))
    table = []
    for held in column:
        line = [held]
        for j in range(inner - 1):
            sent = later(held, *inner_after) if j == 0 and inner_after else line[-1]
            line.append(ring_inner(sent, axis, outer, inner))
        table.append(line)
    return table


def gather_inner_first(block, axis, outer, inner, outer_after=()):
    line = [block]
    for _ in range(inner - 1):
        line.append(ring_inner(line[-1], axis, outer, inner))
    column = [jnp.concatenate(line, axis=0) if inner > 1 else block]
    for k in range(outer - 2):
        sent = later(column[0], *outer_after) if k == 0 and outer_after else column[-1]
        column.append(ring_outer(sent, axis, outer, inner))
    return column


def source_of(axis, outer, inner, k, j):
    me = lax.axis_index(axis)
    return (me // inner + outer - k) % outer * inner + (me % inner + inner - j) % inner


def placed(table, axis, outer, inner):
    depth = table[0][0].shape[0]
    whole = jnp.zeros((depth * outer * inner,) + table[0][0].shape[1:], table[0][0].dtype)
    for k in range(outer):
        for j in range(inner):
            start = source_of(axis, outer, inner, k, j) * depth
            whole = lax.dynamic_update_slice_in_dim(whole, table[k][j], start, 0)
    return whole


def scatter_sum(partial, axis, outer, inner):
    rows, columns = partial.shape
    me = lax.axis_index(axis)
    out_at, in_at = me // inner, me % inner
    cut = partial.reshape(outer, inner, rows // (outer * inner), columns)
    kept = lax.dynamic_index_in_dim(cut, in_at, 1, keepdims=False).astype(jnp.float32)
    for by in range(1, inner):
        sent = lax.dynamic_index_in_dim(cut, (in_at + by) % inner, 1, keepdims=False)
        kept = kept + ring_inner(sent.astype(jnp.bfloat16), axis, outer, inner, by).astype(jnp.float32)
    total = lax.dynamic_index_in_dim(kept, out_at, 0, keepdims=False)
    for by in range(1, outer):
        sent = lax.dynamic_index_in_dim(kept, (out_at + by) % outer, 0, keepdims=False)
        total = total + ring_outer(sent.astype(jnp.bfloat16), axis, outer, inner, by).astype(jnp.float32)
    return total


def extended_2(cells, sides, width):
    for axis, dim in sides:
        count = lax.axis_size(axis)
        ends = count - 1
        head = lax.slice_in_dim(cells, 0, width, axis=dim)
        tail = lax.slice_in_dim(cells, cells.shape[dim] - width, cells.shape[dim], axis=dim)
        cells = jnp.concatenate(
            [
                lax.ppermute(tail, axis, [(i, (i + 1) % count) for i in range(ends)]),
                cells,
                lax.ppermute(head, axis, [((i + 1) % count, i) for i in range(ends)]),
            ],
            axis=dim,
        )
    return cells


def band_blocks(padded, block_count, window_rows):
    row_block = padded.reshape((block_count + 2, window_rows) + padded.shape[1:])
    return jnp.concatenate([row_block[:-2], row_block[1:-1], row_block[2:]], axis=1)


def normalize(stream, gain):
    stream_f = stream.astype(jnp.float32)
    scale = lax.rsqrt(jnp.mean(stream_f * stream_f, axis=-1, keepdims=True) + norm_epsilon)
    return (stream_f * scale * gain).astype(jnp.bfloat16)


def attend(queries, keys_values, sink_logits, doc_ids, offset):
    local_rows = queries.shape[0]
    kv_local = queries.shape[1]
    head_dim = HEAD_DIM
    group_size = queries.shape[2] // head_dim
    window_rows = WINDOW
    block_count = local_rows // window_rows
    padded = extended_2(keys_values, (("sp", 0),), window_rows)
    blocks = band_blocks(padded, block_count, window_rows)
    key_blocks = blocks[..., :head_dim]
    value_blocks = blocks[..., head_dim:]
    query_blocks = queries.reshape(block_count, window_rows, kv_local, group_size, head_dim)
    scores = jnp.einsum(
        "nqkgd,nskd->nkgqs", query_blocks, key_blocks, preferred_element_type=jnp.float32
    ) * head_dim ** (-0.5)
    padded_docs = jnp.pad(doc_ids, window_rows, constant_values=-1)
    near_docs = lax.dynamic_slice_in_dim(padded_docs, offset, local_rows + 2 * window_rows)
    key_docs = band_blocks(near_docs, block_count, window_rows)
    query_docs = near_docs[window_rows : window_rows + local_rows].reshape(block_count, window_rows)
    distance = jnp.arange(window_rows)[:, None] + window_rows - jnp.arange(3 * window_rows)[None, :]
    allowed = (jnp.abs(distance) <= WINDOW)[None] & (query_docs[:, :, None] == key_docs[:, None, :])
    scores = jnp.where(allowed[:, None, None], scores, masked_score)
    sink_part = sink_logits[None, :, :, None, None]
    top_score = jnp.maximum(jnp.max(scores, axis=-1, keepdims=True), sink_part)
    exp_scores = jnp.exp(scores - top_score)
    denominator = jnp.sum(exp_scores, axis=-1, keepdims=True) + jnp.exp(sink_part - top_score)
    probs = (exp_scores / denominator).astype(jnp.bfloat16)
    result = jnp.einsum(
        "nkgqs,nskd->nqkgd", probs, value_blocks, preferred_element_type=jnp.float32
    )
    return result.reshape(local_rows, kv_local * group_size * head_dim).astype(jnp.bfloat16)


def on_device(
    queries,
    keys_values,
    sink_logits,
    doc_ids,
    residual,
    out_weight,
    ffn_gain,
    gate_weight,
    value_weight,
    conv_taps,
    down_weight,
):
    local_rows = queries.shape[0]
    offset = lax.axis_index("sp") * local_rows
    tp_count = lax.axis_size("tp")
    sp_count = lax.axis_size("sp")
    part_rows = local_rows // tp_count
    row_start = lax.axis_index("tp") * part_rows
    hidden_units = gate_weight.shape[1]
    half = down_weight.shape[0] // 2
    sp_outer, sp_inner = factors(sp_count)
    tp_inner = 2 if tp_count % 2 == 0 else 1
    tp_outer = tp_count // tp_inner
    sp_ring = ("sp", sp_outer, sp_inner)
    tp_ring = ("tp", tp_outer, tp_inner)

    both_table = gather_outer_first(jnp.concatenate([gate_weight, value_weight], axis=1), *sp_ring)
    near_end = max(sp_outer - 2, 0)
    first_table = gather_outer_first(
        down_weight[:half], *sp_ring, (both_table[near_end][0],), (both_table[-1][-1],)
    )
    last_column = gather_inner_first(down_weight[half:], *sp_ring, (first_table[near_end][0],))
    out_table = gather_outer_first(out_weight, *tp_ring)
    out_whole = jnp.concatenate([block for line in out_table for block in line], axis=0)

    attended = attend(queries, keys_values, sink_logits, doc_ids, offset)
    attended_table = gather_outer_first(attended, *tp_ring)
    attended_whole = jnp.concatenate([block for line in attended_table for block in line], axis=1)
    projected = jnp.dot(attended_whole, out_whole, preferred_element_type=jnp.float32)
    stream = (residual.astype(jnp.float32) + projected).astype(jnp.bfloat16)
    normed = normalize(stream, ffn_gain)
    stream_rows = lax.dynamic_slice_in_dim(stream, row_start, part_rows, 0)

    before = lax.ppermute(normed[-1:], "sp", [(i, i + 1) for i in range(sp_count - 1)])
    after = lax.ppermute(normed[:1], "sp", [(i + 1, i) for i in range(sp_count - 1)])
    edges = jnp.pad(jnp.concatenate([before, after], axis=0), ((0, 14), (0, 0)))

    both_whole = placed(both_table, *sp_ring)
    both_pre = jnp.dot(normed, both_whole, preferred_element_type=jnp.float32)
    if sp_outer > 1:
        last_column = list(lax.optimization_barrier((*last_column, both_pre))[:-1])
        last_column.append(ring_outer(last_column[-1], *sp_ring))
    gate_stored = both_pre[:, :hidden_units].astype(jnp.bfloat16)
    value_pre = both_pre[:, hidden_units:]
    edge_gate = jnp.dot(edges, both_whole[:, :hidden_units], preferred_element_type=jnp.float32)
    edge_gate = edge_gate.astype(jnp.bfloat16).astype(jnp.float32)
    gate_f = gate_stored.astype(jnp.float32)
    row = lax.broadcasted_iota(jnp.int32, (local_rows, 1), 0)
    gate_before = jnp.where(row == 0, edge_gate[0:1], jnp.roll(gate_f, 1, axis=0))
    gate_after = jnp.where(row == local_rows - 1, edge_gate[1:2], jnp.roll(gate_f, -1, axis=0))
    padded_docs = jnp.pad(doc_ids, 1, constant_values=-1)
    near_docs = lax.dynamic_slice_in_dim(padded_docs, offset, local_rows + 2)
    prev_same = (near_docs[1:-1] == near_docs[:-2]).astype(jnp.float32)[:, None]
    next_same = (near_docs[1:-1] == near_docs[2:]).astype(jnp.float32)[:, None]
    conved = (
        conv_taps[0] * gate_before * prev_same
        + conv_taps[1] * gate_f
        + conv_taps[2] * gate_after * next_same
    )
    hidden = (jax.nn.gelu(conved, approximate=True) * value_pre).astype(jnp.bfloat16)

    def partial_of(rows):
        return lax.dot_general(hidden, rows, contract_last, preferred_element_type=jnp.float32)

    first_partial = partial_of(placed(first_table, *sp_ring))
    first = scatter_sum(first_partial, *tp_ring)
    early_rows = jnp.concatenate(last_column[:-1] or last_column, axis=0)
    last_parts = scatter_sum(partial_of(later(early_rows, first_partial)), *tp_ring)
    if sp_outer > 1:
        late = scatter_sum(partial_of(last_column[-1]), *tp_ring)
        last_parts = jnp.concatenate([last_parts, late], axis=1)
    last = jnp.zeros_like(first)
    for k in range(sp_outer):
        for j in range(sp_inner):
            at = (k * sp_inner + j) * half
            start = source_of("sp", sp_outer, sp_inner, k, j) * half
            last = lax.dynamic_update_slice_in_dim(last, last_parts[:, at : at + half], start, 1)
    lowered = jnp.stack(
        [first.reshape(part_rows, sp_count, half), last.reshape(part_rows, sp_count, half)], axis=2
    ).reshape(part_rows, 2 * half * sp_count)
    return (stream_rows.astype(jnp.float32) + lowered).astype(jnp.bfloat16)


def solution(mesh):
    in_specs = (
        P("sp", "tp", None),
        P("sp", "tp", None),
        P("tp", None),
        P(),
        P("sp", None),
        P("tp", None),
        P(),
        P("sp", "tp"),
        P("sp", "tp"),
        P(None, "tp"),
        P("sp", "tp"),
    )
    out_specs = P(("sp", "tp"), None)
    return jax.shard_map(
        on_device, mesh=mesh, in_specs=in_specs, out_specs=out_specs, check_vma=False
    )
```
